512 devices in a mesh: fs: 64 (over z, y), tp: 8 (over x, core).
Axes of the slice: x: 4, y: 8, z: 8, core: 2. Of those that a mesh axis runs over, the one named last changes fastest.
Arguments:
- prompt: bfloat16 [20480, 2048], P('fs', 'tp'), may hold values from -6 to 6
- norm_gain: float32 [2048], P('fs'), may hold values from 0.1 to 1.9
- gate_master: float32 [2048, 3072], P('fs', 'tp'), may hold values from -0.125 to 0.125
- up_master: float32 [2048, 3072], P('fs', 'tp'), may hold values from -0.125 to 0.125
- down_master: float32 [2048, 3072], P('fs', 'tp'), may hold values from -0.109375 to 0.109375
Outputs:
- gate_new: bfloat16 [3072, 2048], P('tp')
- up_new: bfloat16 [3072, 2048], P('tp')
- down_new: bfloat16 [3072, 2048], P('tp')
- mixed: bfloat16 [2048, 20480], P('tp', 'fs')
The draws below stay inside these ranges and needn't reach their ends.
All inputs are finite; a program needn't handle non-finite values.
Results may differ from the reference program's by a relative error of at most 0.0082.
Values may be sent and summed in bfloat16 or wider, within the bound.
No kernel may reach another device: no remote copies, remote signals or barrier semaphores. Data moves between devices by JAX's collectives and lax.ppermute only.
A program may use at most 64 MiB of HBM per device.

```python
import jax
import jax.numpy as jnp
from jax import lax

D = 2048
FF = 3072
TOKENS = 20480


def block_levels(rng, shape, shards, smallest, high):
    factor_of, own = 1.0, jax.random.fold_in(rng, 6)
    for position, parts in shards:
        draws = jnp.exp(jax.random.uniform(jax.random.fold_in(own, position), (parts,), jnp.float32, smallest / len(shards), high / len(shards)))
        factor_of = factor_of * jnp.repeat(draws, shape[position] // parts).reshape([-1 if axis == position else 1 for axis in range(len(shape))])
    return factor_of


def normal_values(rng, extent, spread, limit, pieces=(), dtype=jnp.bfloat16):
    values = spread * jax.random.normal(rng, extent, jnp.float32)
    if pieces:
        values = values * block_levels(rng, extent, pieces, -0.22, 0.18)
    return jnp.clip(values, -limit, limit).astype(dtype)


def setup_inputs(seed: int = 0) -> dict:
    keys = jax.random.split(jax.random.key(seed), 6)
    return {
        "prompt": normal_values(keys[0], (TOKENS, D), 1.0, 6.0, ((0, 64), (1, 8))),
        "norm_gain": jnp.clip(1.0 + 0.18 * jax.random.normal(keys[1], (D,), jnp.float32), 0.1, 1.9),
        "gate_master": normal_values(keys[2], (D, FF), D ** -0.5, 0.125, ((0, 64), (1, 8)), jnp.float32),
        "up_master": normal_values(keys[3], (D, FF), D ** -0.5, 0.125, ((0, 64), (1, 8)), jnp.float32),
        "down_master": normal_values(keys[4], (D, FF), FF ** -0.5, 0.109375, ((0, 64), (1, 8)), jnp.float32),
    }


def reference(prompt, norm_gain, gate_master, up_master, down_master):
    gain_col = norm_gain[:, None]
    gate_new = (gate_master * gain_col).astype(jnp.bfloat16).T
    up_new = (up_master * gain_col).astype(jnp.bfloat16).T
    down_new = down_master.astype(jnp.bfloat16).T
    values = prompt.astype(jnp.float32)
    normed = (values * lax.rsqrt(lax.optimization_barrier(jnp.mean(values * values, axis=1, keepdims=True)) + 1e-06)).astype(jnp.bfloat16)
    gate = jnp.dot(normed, gate_new.T, preferred_element_type=jnp.float32)
    up = jnp.dot(normed, up_new.T, preferred_element_type=jnp.float32)
    hidden = (jax.nn.silu(gate) * up).astype(jnp.bfloat16)
    mixed = jnp.dot(down_new.T, hidden.T, preferred_element_type=jnp.float32).astype(jnp.bfloat16)
    return (gate_new, up_new, down_new, mixed)
```

```python
import jax
import jax.numpy as jnp
from jax import lax
from jax.sharding import PartitionSpec as P

SCALE = 2.0**18


def on_device(prompt, norm_gain, gate_master, up_master, down_master):
    gain_col = norm_gain[:, None]
    parts = [gate_master * gain_col, up_master * gain_col, down_master]
    low = jnp.concatenate([(lax.reduce_precision(p, 8, 7) * SCALE).astype(jnp.float16) for p in parts], axis=1)
    whole = lax.all_to_all(jnp.broadcast_to(prompt, (8, *prompt.shape)), "tp", 0, 0, tiled=True)
    filled = lax.all_gather(low, "fs", axis=0, tiled=True)
    back = (filled.astype(jnp.float32) * (1 / SCALE)).astype(jnp.bfloat16)
    gate_w, up_w, down_w = back[:, :384], back[:, 384:768], back[:, 768:]
    values = whole.transpose(1, 0, 2).reshape(320, 2048).astype(jnp.float32)
    normed = (values * lax.rsqrt(jnp.mean(values * values, axis=1, keepdims=True) + 1e-06)).astype(jnp.bfloat16)
    gate = jnp.dot(normed, gate_w, preferred_element_type=jnp.float32)
    up = jnp.dot(normed, up_w, preferred_element_type=jnp.float32)
    hidden = (jax.nn.silu(gate) * up).astype(jnp.bfloat16)
    partial = lax.dot_general(down_w, hidden, (((1,), (1,)), ((), ())), preferred_element_type=jnp.float32).astype(jnp.bfloat16)
    arrived = lax.all_to_all(partial.reshape(8, 256, 320), "tp", 0, 0, tiled=True)
    mixed = arrived.astype(jnp.float32).sum(axis=0).astype(jnp.bfloat16)
    return gate_w.T, up_w.T, down_w.T, mixed


def solution(mesh):
    placed = (P("fs", "tp"), P("fs"), P("fs", "tp"), P("fs", "tp"), P("fs", "tp"))
    return jax.shard_map(
        on_device,
        mesh=mesh,
        in_specs=placed,
        out_specs=(P("tp", None), P("tp", None), P("tp", None), P("tp", "fs")),
        check_vma=False,
    )
```

```python
import jax
import jax.numpy as jnp
from jax import lax
from jax.experimental import pallas as pl
from jax.experimental.pallas import tpu as pltpu
from jax.sharding import PartitionSpec as P

SIDE = 8
SCALE = 2.0**18
VMEM = pl.BlockSpec(memory_space=pltpu.VMEM)
FAR = pl.BlockSpec(memory_space=pltpu.HBM)
SMEM = pl.BlockSpec(memory_space=pltpu.SMEM)


def struct(shape, dtype=jnp.bfloat16):
    return jax.ShapeDtypeStruct(shape, dtype)


def hidden_kernel(core, x_ref, near_ref, other_ref, mine_ref, kept_ref, low_ref, normed_ref, sems, keep_sem):
    slabs, tokens, width = x_ref.shape
    cols = low_ref.shape[1] // 3
    rows = low_ref.shape[0] // (SIDE * SIDE)
    outer, inner = jnp.where(core[0] == 0, SIDE, 1), jnp.where(core[0] == 0, 1, SIDE)
    copies = []
    for z in range(SIDE):
        for y in range(SIDE):
            row = pl.multiple_of((z * outer + y * inner) * rows, rows)
            to = low_ref.at[pl.ds((z * SIDE + y) * rows, rows)]
            copies.append(pltpu.make_async_copy(near_ref.at[pl.ds(row, rows)], to, sems.at[z, y]))
            copies[-1].start()
    squares = jnp.zeros((tokens, width), jnp.float32)
    for s in range(slabs):
        x = x_ref[s].astype(jnp.float32)
        squares += x * x
    inverse = lax.rsqrt(jnp.sum(squares, axis=1, keepdims=True) / (slabs * width) + 1e-06)
    for s in range(slabs):
        normed_ref[:, s * width : (s + 1) * width] = (x_ref[s].astype(jnp.float32) * inverse).astype(jnp.bfloat16)
    for copy in copies:
        copy.wait()
    keep = pltpu.make_async_copy(low_ref, kept_ref, keep_sem)
    keep.start()
    gate = jnp.dot(normed_ref[...], low_ref[:, :cols], preferred_element_type=jnp.float32)
    up = jnp.dot(normed_ref[...], low_ref[:, cols : 2 * cols], preferred_element_type=jnp.float32)
    hidden = (gate / (1 + jnp.exp(-gate)) * up).astype(jnp.bfloat16)

    def share(slab):
        down = low_ref[pl.ds(pl.multiple_of(slab * width, width), width), 2 * cols :]
        return lax.dot_general(hidden, down, (((1,), (1,)), ((), ())), preferred_element_type=jnp.float32)

    for k in range(slabs // 2):
        other_ref[k] = share(2 * k + 1 - core[0]).astype(jnp.bfloat16)
        mine_ref[k] = share(2 * k + core[0])
    keep.wait()


def pair_kernel(mine_ref, got_ref, out_ref):
    out_ref[...] = (mine_ref[...] + got_ref[...].astype(jnp.float32)).astype(jnp.bfloat16)


def turn_kernel(low_ref, gate_ref, up_ref, down_ref):
    cols = gate_ref.shape[0]
    for k, ref in enumerate((gate_ref, up_ref, down_ref)):
        ref[...] = low_ref[:, k * cols : (k + 1) * cols].T


def sum_kernel(parts_ref, out_ref):
    total = parts_ref[0].astype(jnp.float32)
    for k in range(1, parts_ref.shape[0]):
        total += parts_ref[k].astype(jnp.float32)
    out_ref[...] = total.astype(jnp.bfloat16)


def device(z, y, t, tp):
    return (z * SIDE + y) * tp + t


def lines(tp, even, odd):
    groups = []
    for t in range(tp):
        for o in range(SIDE):
            along = (odd if t % 2 else even) == "y"
            groups.append([device(o, i, t, tp) if along else device(i, o, t, tp) for i in range(SIDE)])
    return groups


def on_device(prompt, norm_gain, gate_master, up_master, down_master):
    tp, fs = lax.axis_size("tp"), lax.axis_size("fs")
    tokens, width = prompt.shape
    rows, cols = gate_master.shape
    every = ("fs", "tp")
    gain_col = norm_gain[:, None]
    parts = [gate_master * gain_col, up_master * gain_col, down_master]
    sent = jnp.concatenate([(lax.reduce_precision(p, 8, 7) * SCALE).astype(jnp.float16) for p in parts], axis=1)
    whole = lax.all_to_all(jnp.broadcast_to(prompt, (tp, *prompt.shape)), "tp", 0, 0, tiled=True)
    own = lax.all_to_all(
        jnp.broadcast_to(sent, (SIDE, *sent.shape)), every, 0, 0, tiled=True, axis_index_groups=lines(tp, "y", "z")
    )
    filled = lax.all_gather(own.reshape(SIDE * rows, 3 * cols), every, axis=0, tiled=True, axis_index_groups=lines(tp, "z", "y"))
    near = (filled.astype(jnp.float32) * (1 / SCALE)).astype(jnp.bfloat16)
    core = (lax.axis_index("tp") % 2).astype(jnp.int32)[None]
    full = (rows * fs, 3 * cols)
    block = (tp // 2, tokens, width)
    other, mine, low = pl.pallas_call(
        hidden_kernel,
        out_shape=(struct(block), struct(block, jnp.float32), struct(full)),
        in_specs=[SMEM, VMEM, FAR],
        out_specs=(VMEM, VMEM, FAR),
        scratch_shapes=[
            pltpu.VMEM(full, jnp.bfloat16),
            pltpu.VMEM((tokens, tp * width), jnp.bfloat16),
            pltpu.SemaphoreType.DMA((SIDE, SIDE)),
            pltpu.SemaphoreType.DMA,
        ],
        compiler_params=pltpu.CompilerParams(vmem_limit_bytes=50 << 20),
    )(core, whole, near)
    got = lax.ppermute(other, "tp", [(t, t ^ 1) for t in range(tp)])
    paired = pl.pallas_call(
        pair_kernel,
        out_shape=struct(block),
        in_specs=[VMEM, VMEM],
        out_specs=VMEM,
        compiler_params=pltpu.CompilerParams(vmem_limit_bytes=8 << 20),
    )(mine, got)
    chips = [[t for t in range(c, tp, 2)] for c in range(2)]
    summed = lax.all_to_all(paired, "tp", 0, 0, tiled=True, axis_index_groups=chips)
    turned = struct((cols, rows * fs))
    gate_new, up_new, down_new = pl.pallas_call(
        turn_kernel,
        out_shape=(turned, turned, turned),
        grid=(rows * fs // width,),
        in_specs=[pl.BlockSpec((width, 3 * cols), lambda s: (s, 0))],
        out_specs=[pl.BlockSpec((cols, width), lambda s: (0, s))] * 3,
        compiler_params=pltpu.CompilerParams(vmem_limit_bytes=58 << 20),
        cost_estimate=pl.CostEstimate(flops=2 * 10**9, bytes_accessed=12 * rows * fs * cols, transcendentals=0),
    )(low)
    mixed = pl.pallas_call(
        sum_kernel,
        out_shape=struct((tokens, width)),
        in_specs=[VMEM],
        out_specs=VMEM,
        compiler_params=pltpu.CompilerParams(vmem_limit_bytes=6 << 20),
    )(summed)
    return gate_new, up_new, down_new, mixed.T


def solution(mesh):
    placed = (P("fs", "tp"), P("fs"), P("fs", "tp"), P("fs", "tp"), P("fs", "tp"))
    return jax.shard_map(
        on_device,
        mesh=mesh,
        in_specs=placed,
        out_specs=(P("tp", None), P("tp", None), P("tp", None), P("tp", "fs")),
        check_vma=False,
    )
```

```python
import jax
import jax.numpy as jnp
from jax import lax
from jax.experimental import pallas as pl
from jax.experimental.pallas import tpu as pltpu
from jax.sharding import PartitionSpec as P


SIDE = 8
SCALE = 2.0**18
VMEM = pl.BlockSpec(memory_space=pltpu.VMEM)
FAR = pl.BlockSpec(memory_space=pltpu.HBM)
SMEM = pl.BlockSpec(memory_space=pltpu.SMEM)


def struct(shape, dtype=jnp.bfloat16):
    return jax.ShapeDtypeStruct(shape, dtype)


def strides(core):
    return jnp.where(core == 0, 1, SIDE), jnp.where(core == 0, SIDE, 1)


def hidden_kernel(core, x_ref, near_ref, other_ref, mine_ref, low_ref, normed_ref, sems):
    slabs, tokens, width = x_ref.shape
    cols = low_ref.shape[1] // 3
    rows = low_ref.shape[0] // (SIDE * SIDE)
    along_z, along_y = strides(core[0])
    copies = []
    for z in range(SIDE):
        for y in range(SIDE):
            row = pl.multiple_of((z * along_z + y * along_y) * rows, rows)
            to = low_ref.at[pl.ds((z * SIDE + y) * rows, rows)]
            copies.append(pltpu.make_async_copy(near_ref.at[pl.ds(row, rows)], to, sems.at[z, y]))
            copies[-1].start()
    squares = jnp.zeros((tokens, width), jnp.float32)
    for s in range(slabs):
        x = x_ref[s].astype(jnp.float32)
        squares += x * x
    inverse = lax.rsqrt(jnp.sum(squares, axis=1, keepdims=True) / (slabs * width) + 1e-06)
    for s in range(slabs):
        normed_ref[:, s * width : (s + 1) * width] = (x_ref[s].astype(jnp.float32) * inverse).astype(jnp.bfloat16)
    both, half = 0.0, slabs * width // 2
    for part in range(2):
        for copy in copies[part * SIDE * SIDE // 2 : (part + 1) * SIDE * SIDE // 2]:
            copy.wait()
        ks = slice(part * half, (part + 1) * half)
        both += jnp.dot(normed_ref[:, ks], low_ref[ks, : 2 * cols], preferred_element_type=jnp.float32)
    gate, up = both[:, :cols], both[:, cols:]
    hidden = (gate / (1 + jnp.exp(-gate)) * up).astype(jnp.bfloat16)

    def share(slab):
        down = low_ref[pl.ds(pl.multiple_of(slab * width, width), width), 2 * cols :]
        return lax.dot_general(hidden, down, (((1,), (1,)), ((), ())), preferred_element_type=jnp.float32)

    for k in range(slabs // 2):
        other_ref[k] = share(2 * k + 1 - core[0]).astype(jnp.bfloat16)
        mine_ref[k] = share(2 * k + core[0])


def pair_kernel(mine_ref, got_ref, out_ref):
    out_ref[...] = (mine_ref[...] + got_ref[...].astype(jnp.float32)).astype(jnp.bfloat16)


def turn_kernel(core, *refs):
    pieces, outs = refs[:SIDE], refs[SIDE:]
    cols = outs[0].shape[0]
    for k, out in enumerate(outs):
        slab = jnp.concatenate([piece[:, k * cols : (k + 1) * cols] for piece in pieces], axis=0)
        out[...] = slab.T


def sum_kernel(parts_ref, out_ref):
    total = parts_ref[0].astype(jnp.float32)
    for k in range(1, parts_ref.shape[0]):
        total += parts_ref[k].astype(jnp.float32)
    out_ref[...] = total.astype(jnp.bfloat16)


def device(z, y, t, tp):
    return (z * SIDE + y) * tp + t


def lines(tp, even, odd):
    groups = []
    for t in range(tp):
        for o in range(SIDE):
            along = (odd if t % 2 else even) == "y"
            groups.append([device(o, i, t, tp) if along else device(i, o, t, tp) for i in range(SIDE)])
    return groups


def on_device(prompt, norm_gain, gate_master, up_master, down_master):
    tp, fs = lax.axis_size("tp"), lax.axis_size("fs")
    tokens, width = prompt.shape
    rows, cols = gate_master.shape
    every = ("fs", "tp")
    gain_col = norm_gain[:, None]
    parts = [gate_master * gain_col, up_master * gain_col, down_master]
    sent = jnp.concatenate([(lax.reduce_precision(p, 8, 7) * SCALE).astype(jnp.float16) for p in parts], axis=1)
    copies = jnp.broadcast_to(sent, (SIDE, *sent.shape))
    own = lax.all_to_all(copies, every, 0, 0, tiled=True, axis_index_groups=lines(tp, "z", "y"))
    prompts = jnp.broadcast_to(prompt, (tp, *prompt.shape))
    whole = lax.all_to_all(prompts, "tp", 0, 0, tiled=True)
    filled = lax.all_gather(own.reshape(SIDE * rows, 3 * cols), every, axis=0, tiled=True, axis_index_groups=lines(tp, "y", "z"))
    near = (filled.astype(jnp.float32) * (1 / SCALE)).astype(jnp.bfloat16)
    core = (lax.axis_index("tp") % 2).astype(jnp.int32)[None]
    full = (rows * fs, 3 * cols)
    block = (tp // 2, tokens, width)
    other, mine = pl.pallas_call(
        hidden_kernel,
        out_shape=(struct(block), struct(block, jnp.float32)),
        in_specs=[SMEM, VMEM, FAR],
        out_specs=(VMEM, VMEM),
        scratch_shapes=[
            pltpu.VMEM(full, jnp.bfloat16),
            pltpu.VMEM((tokens, tp * width), jnp.bfloat16),
            pltpu.SemaphoreType.DMA((SIDE, SIDE)),
        ],
        compiler_params=pltpu.CompilerParams(vmem_limit_bytes=50 << 20),
    )(core, whole, near)
    got = lax.ppermute(other, "tp", [(t, t ^ 1) for t in range(tp)])
    paired = pl.pallas_call(
        pair_kernel,
        out_shape=struct(block),
        in_specs=[VMEM, VMEM],
        out_specs=VMEM,
        compiler_params=pltpu.CompilerParams(vmem_limit_bytes=8 << 20),
    )(mine, got)
    chips = [[t for t in range(c, tp, 2)] for c in range(2)]
    summed = lax.all_to_all(paired, "tp", 0, 0, tiled=True, axis_index_groups=chips)
    turned = struct((cols, rows * fs))

    def piece(y):
        def index(z, core):
            along_z, along_y = strides(core[0])
            return z * along_z + y * along_y, 0

        return pl.BlockSpec((rows, 3 * cols), index)

    gate_new, up_new, down_new = pl.pallas_call(
        turn_kernel,
        out_shape=(turned, turned, turned),
        grid_spec=pltpu.PrefetchScalarGridSpec(
            num_scalar_prefetch=1,
            grid=(SIDE,),
            in_specs=[piece(y) for y in range(SIDE)],
            out_specs=[pl.BlockSpec((cols, SIDE * rows), lambda z, core: (0, z))] * 3,
        ),
        compiler_params=pltpu.CompilerParams(vmem_limit_bytes=58 << 20),
        cost_estimate=pl.CostEstimate(flops=2 * 10**9, bytes_accessed=12 * rows * fs * cols, transcendentals=0),
    )(core, *[near] * SIDE)
    mixed = pl.pallas_call(
        sum_kernel,
        out_shape=struct((tokens, width)),
        in_specs=[VMEM],
        out_specs=VMEM,
        compiler_params=pltpu.CompilerParams(vmem_limit_bytes=6 << 20),
    )(summed)
    return gate_new, up_new, down_new, mixed.T


def solution(mesh):
    placed = (P("fs", "tp"), P("fs"), P("fs", "tp"), P("fs", "tp"), P("fs", "tp"))
    return jax.shard_map(
        on_device,
        mesh=mesh,
        in_specs=placed,
        out_specs=(P("tp", None), P("tp", None), P("tp", None), P("tp", "fs")),
        check_vma=False,
    )
```

```python
import jax
import jax.numpy as jnp
from jax import lax
from jax.experimental import pallas as pl
from jax.experimental.pallas import tpu as pltpu
from jax.sharding import PartitionSpec as P


SIDE = 8
SCALE = 2.0**18
VMEM = pl.BlockSpec(memory_space=pltpu.VMEM)
SMEM = pl.BlockSpec(memory_space=pltpu.SMEM)


def struct(shape, dtype=jnp.bfloat16):
    return jax.ShapeDtypeStruct(shape, dtype)


def strides(core):
    return jnp.where(core == 0, 1, SIDE), jnp.where(core == 0, SIDE, 1)


def hidden_kernel(me, *refs):
    pairs, (near_ref, other_ref, mine_ref, normed_ref) = refs[: len(refs) - 4], refs[len(refs) - 4 :]
    chips = len(pairs)
    _, tokens, width = pairs[0].shape
    cols = near_ref.shape[-1] // 3
    core = lax.rem(me[0], 2)
    along_z, along_y = strides(core)
    squares = jnp.zeros((tokens, width), jnp.float32)
    for pair in pairs:
        for k in range(2):
            x = pair[k].astype(jnp.float32)
            squares += x * x
    inverse = lax.rsqrt(jnp.sum(squares, axis=1, keepdims=True) / (2 * chips * width) + 1e-06)
    for step, pair in enumerate(pairs):
        chip = lax.rem(me[0] // 2 + chips - step, chips)
        for k in range(2):
            slab = 2 * chip + (core if k == 0 else 1 - core)
            normed_ref[slab] = (pair[k].astype(jnp.float32) * inverse).astype(jnp.bfloat16)

    def weights(slab, columns):
        return jnp.concatenate([near_ref[slab * along_z + y * along_y, :, columns] for y in range(SIDE)], axis=0)

    both = 0.0
    for z in range(SIDE):
        both += jnp.dot(normed_ref[z], weights(z, slice(0, 2 * cols)), preferred_element_type=jnp.float32)
    gate, up = both[:, :cols], both[:, cols:]
    hidden = (gate / (1 + jnp.exp(-gate)) * up).astype(jnp.bfloat16)

    def share(slab):
        down = weights(slab, slice(2 * cols, 3 * cols))
        return lax.dot_general(hidden, down, (((1,), (1,)), ((), ())), preferred_element_type=jnp.float32)

    for k in range(chips):
        other_ref[k] = share(2 * k + 1 - core).astype(jnp.bfloat16)
        mine_ref[k] = share(2 * k + core)


def pair_kernel(mine_ref, got_ref, out_ref):
    out_ref[...] = (mine_ref[...] + got_ref[...].astype(jnp.float32)).astype(jnp.bfloat16)


def turn_kernel(me, *refs):
    pieces, outs = refs[:SIDE], refs[SIDE:]
    cols = outs[0].shape[0]
    for k, out in enumerate(outs):
        slab = jnp.concatenate([piece[:, k * cols : (k + 1) * cols] for piece in pieces], axis=0)
        out[...] = slab.T


def sum_kernel(parts_ref, out_ref):
    total = parts_ref[0].astype(jnp.float32)
    for k in range(1, parts_ref.shape[0]):
        total += parts_ref[k].astype(jnp.float32)
    out_ref[...] = total.astype(jnp.bfloat16)


def device(z, y, t, tp):
    return (z * SIDE + y) * tp + t


def lines(tp, even, odd):
    groups = []
    for t in range(tp):
        for o in range(SIDE):
            along = (odd if t % 2 else even) == "y"
            groups.append([device(o, i, t, tp) if along else device(i, o, t, tp) for i in range(SIDE)])
    return groups


def on_device(prompt, norm_gain, gate_master, up_master, down_master):
    tp, fs = lax.axis_size("tp"), lax.axis_size("fs")
    tokens, width = prompt.shape
    rows, cols = gate_master.shape
    every = ("fs", "tp")
    gain_col = norm_gain[:, None]
    parts = [gate_master * gain_col, up_master * gain_col, down_master]
    sent = jnp.concatenate([(lax.reduce_precision(p, 8, 7) * SCALE).astype(jnp.float16) for p in parts], axis=1)
    copies = jnp.broadcast_to(sent, (SIDE, *sent.shape))
    own = lax.all_to_all(copies, every, 0, 0, tiled=True, axis_index_groups=lines(tp, "z", "y"))
    partner = lax.ppermute(prompt, "tp", [(t, t ^ 1) for t in range(tp)])
    pairs = [jnp.stack([prompt, partner])]
    for step in range(1, tp // 2):
        pairs.append(lax.ppermute(pairs[0], "tp", [(t, (t + 2 * step) % tp) for t in range(tp)]))
    filled = lax.all_gather(own.reshape(SIDE * rows, 3 * cols), every, axis=0, tiled=True, axis_index_groups=lines(tp, "y", "z"))
    near = (filled.astype(jnp.float32) * (1 / SCALE)).astype(jnp.bfloat16)
    me = lax.axis_index("tp").astype(jnp.int32)[None]
    block = (tp // 2, tokens, width)
    other, mine = pl.pallas_call(
        hidden_kernel,
        out_shape=(struct(block), struct(block, jnp.float32)),
        in_specs=[SMEM] + [VMEM] * (tp // 2 + 1),
        out_specs=(VMEM, VMEM),
        scratch_shapes=[pltpu.VMEM((tp, tokens, width), jnp.bfloat16)],
        compiler_params=pltpu.CompilerParams(vmem_limit_bytes=16 << 20),
    )(me, *pairs, near.reshape(SIDE * SIDE, rows, 3 * cols))
    got = lax.ppermute(other, "tp", [(t, t ^ 1) for t in range(tp)])
    paired = pl.pallas_call(
        pair_kernel,
        out_shape=struct(block),
        in_specs=[VMEM, VMEM],
        out_specs=VMEM,
        compiler_params=pltpu.CompilerParams(vmem_limit_bytes=8 << 20),
    )(mine, got)
    chips = [[t for t in range(c, tp, 2)] for c in range(2)]
    summed = lax.all_to_all(paired, "tp", 0, 0, tiled=True, axis_index_groups=chips)
    turned = struct((cols, rows * fs))

    def piece(y):
        def index(z, me):
            along_z, along_y = strides(lax.rem(me[0], 2))
            return z * along_z + y * along_y, 0

        return pl.BlockSpec((rows, 3 * cols), index)

    gate_new, up_new, down_new = pl.pallas_call(
        turn_kernel,
        out_shape=(turned, turned, turned),
        grid_spec=pltpu.PrefetchScalarGridSpec(
            num_scalar_prefetch=1,
            grid=(SIDE,),
            in_specs=[piece(y) for y in range(SIDE)],
            out_specs=[pl.BlockSpec((cols, SIDE * rows), lambda z, me: (0, z))] * 3,
        ),
        compiler_params=pltpu.CompilerParams(vmem_limit_bytes=58 << 20),
        cost_estimate=pl.CostEstimate(flops=2 * 10**9, bytes_accessed=12 * rows * fs * cols, transcendentals=0),
    )(me, *[near] * SIDE)
    mixed = pl.pallas_call(
        sum_kernel,
        out_shape=struct((tokens, width)),
        in_specs=[VMEM],
        out_specs=VMEM,
        compiler_params=pltpu.CompilerParams(vmem_limit_bytes=6 << 20),
    )(summed)
    return gate_new, up_new, down_new, mixed.T


def solution(mesh):
    placed = (P("fs", "tp"), P("fs"), P("fs", "tp"), P("fs", "tp"), P("fs", "tp"))
    return jax.shard_map(
        on_device,
        mesh=mesh,
        in_specs=placed,
        out_specs=(P("tp", None), P("tp", None), P("tp", None), P("tp", "fs")),
        check_vma=False,
    )
```

```python
import jax
import jax.numpy as jnp
from jax import lax
from jax.experimental import pallas as pl
from jax.experimental.pallas import tpu as pltpu
from jax.sharding import PartitionSpec as P


SIDE = 8
SCALE = 2.0**18
VMEM = pl.BlockSpec(memory_space=pltpu.VMEM)
SMEM = pl.BlockSpec(memory_space=pltpu.SMEM)


def struct(shape, dtype=jnp.bfloat16):
    return jax.ShapeDtypeStruct(shape, dtype)


def strides(core):
    return jnp.where(core == 0, 1, SIDE), jnp.where(core == 0, SIDE, 1)


def lift_kernel(prompt_ref, out_ref):
    out_ref[...] = prompt_ref[...]


def stack_kernel(first_ref, second_ref, out_ref):
    out_ref[0] = first_ref[...]
    out_ref[1] = second_ref[...]


def hidden_kernel(me, *refs):
    pairs, (near_ref, other_ref, mine_ref) = refs[: len(refs) - 3], refs[len(refs) - 3 :]
    chips = len(pairs)
    _, tokens, width = pairs[0].shape
    cols = near_ref.shape[-1] // 3
    core = lax.rem(me[0], 2)
    along_z, along_y = strides(core)

    def weights(slab, columns):
        at = [slab * along_z + y * along_y for y in range(SIDE)]
        return jnp.concatenate([near_ref[row, :, columns] for row in at], axis=0)

    squares, both = jnp.zeros((tokens, width), jnp.float32), 0.0
    for step, pair in enumerate(pairs):
        chip = lax.rem(me[0] // 2 + chips - step, chips)
        for k in range(2):
            x = pair[k]
            slab = 2 * chip + (core if k == 0 else 1 - core)
            both += jnp.dot(x, weights(slab, slice(0, 2 * cols)), preferred_element_type=jnp.float32)
            squares += x.astype(jnp.float32) * x.astype(jnp.float32)
    inverse = lax.rsqrt(jnp.sum(squares, axis=1, keepdims=True) / (2 * chips * width) + 1e-06)
    gate, up = both[:, :cols] * inverse, both[:, cols:] * inverse
    hidden = (gate / (1 + jnp.exp(-gate)) * up).astype(jnp.bfloat16)

    def share(slab):
        down = weights(slab, slice(2 * cols, 3 * cols))
        return lax.dot_general(hidden, down, (((1,), (1,)), ((), ())), preferred_element_type=jnp.float32)

    for k in range(chips):
        other_ref[k] = share(2 * k + 1 - core).astype(jnp.bfloat16)
        mine_ref[k] = share(2 * k + core)


def pair_kernel(mine_ref, got_ref, out_ref):
    out_ref[...] = (mine_ref[...] + got_ref[...].astype(jnp.float32)).astype(jnp.bfloat16)


def turn_kernel(me, near_ref, *outs):
    cols = outs[0].shape[0]
    along_z, along_y = strides(lax.rem(me[0], 2))
    at = [pl.program_id(0) * along_z + y * along_y for y in range(SIDE)]
    for k, out in enumerate(outs):
        slab = jnp.concatenate([near_ref[row, :, k * cols : (k + 1) * cols] for row in at], axis=0)
        out[...] = slab.T


def sum_kernel(parts_ref, out_ref):
    total = parts_ref[0].astype(jnp.float32)
    for k in range(1, parts_ref.shape[0]):
        total += parts_ref[k].astype(jnp.float32)
    out_ref[...] = total.astype(jnp.bfloat16)


def device(z, y, t, tp):
    return (z * SIDE + y) * tp + t


def lines(tp, even, odd):
    groups = []
    for t in range(tp):
        for o in range(SIDE):
            along = (odd if t % 2 else even) == "y"
            groups.append([device(o, i, t, tp) if along else device(i, o, t, tp) for i in range(SIDE)])
    return groups


def on_device(prompt, norm_gain, gate_master, up_master, down_master):
    tp, fs = lax.axis_size("tp"), lax.axis_size("fs")
    tokens, width = prompt.shape
    rows, cols = gate_master.shape
    every = ("fs", "tp")
    gain_col = norm_gain[:, None]
    parts = [gate_master * gain_col, up_master * gain_col, down_master]
    sent = jnp.concatenate([(lax.reduce_precision(p, 8, 7) * SCALE).astype(jnp.float16) for p in parts], axis=1)
    copies = jnp.broadcast_to(sent, (SIDE, *sent.shape))
    own = lax.all_to_all(copies, every, 0, 0, tiled=True, axis_index_groups=lines(tp, "z", "y"))
    partner = lax.ppermute(prompt, "tp", [(t, t ^ 1) for t in range(tp)])
    own_prompt = pl.pallas_call(
        lift_kernel,
        out_shape=struct((tokens, width)),
        in_specs=[VMEM],
        out_specs=VMEM,
        compiler_params=pltpu.CompilerParams(vmem_limit_bytes=4 << 20),
    )(prompt)
    pairs = [
        pl.pallas_call(
            stack_kernel,
            out_shape=struct((2, tokens, width)),
            in_specs=[VMEM, VMEM],
            out_specs=VMEM,
            compiler_params=pltpu.CompilerParams(vmem_limit_bytes=4 << 20),
        )(own_prompt, partner)
    ]
    for step in range(1, tp // 2):
        pairs.append(lax.ppermute(pairs[0], "tp", [(t, (t + 2 * step) % tp) for t in range(tp)]))
    filled = lax.all_gather(own.reshape(SIDE * rows, 3 * cols), every, axis=0, tiled=True, axis_index_groups=lines(tp, "y", "z"))
    near = (filled.astype(jnp.float32) * (1 / SCALE)).astype(jnp.bfloat16)
    me = lax.axis_index("tp").astype(jnp.int32)[None]
    block = (tp // 2, tokens, width)
    other, mine = pl.pallas_call(
        hidden_kernel,
        out_shape=(struct(block), struct(block, jnp.float32)),
        in_specs=[SMEM] + [VMEM] * (tp // 2 + 1),
        out_specs=(VMEM, VMEM),
        compiler_params=pltpu.CompilerParams(vmem_limit_bytes=16 << 20),
    )(me, *pairs, near.reshape(SIDE * SIDE, rows, 3 * cols))
    got = lax.ppermute(other, "tp", [(t, t ^ 1) for t in range(tp)])
    paired = pl.pallas_call(
        pair_kernel,
        out_shape=struct(block),
        in_specs=[VMEM, VMEM],
        out_specs=VMEM,
        compiler_params=pltpu.CompilerParams(vmem_limit_bytes=8 << 20),
    )(mine, got)
    chips = [[t for t in range(c, tp, 2)] for c in range(2)]
    summed = lax.all_to_all(paired, "tp", 0, 0, tiled=True, axis_index_groups=chips)
    turned = struct((cols, rows * fs))

    gate_new, up_new, down_new = pl.pallas_call(
        turn_kernel,
        out_shape=(turned, turned, turned),
        grid_spec=pltpu.PrefetchScalarGridSpec(
            num_scalar_prefetch=1,
            grid=(SIDE,),
            in_specs=[VMEM],
            out_specs=[pl.BlockSpec((cols, SIDE * rows), lambda z, me: (0, z))] * 3,
        ),
        compiler_params=pltpu.CompilerParams(vmem_limit_bytes=16 << 20),
        cost_estimate=pl.CostEstimate(flops=2 * 10**9, bytes_accessed=12 * rows * fs * cols, transcendentals=0),
    )(me, near.reshape(SIDE * SIDE, rows, 3 * cols))
    mixed = pl.pallas_call(
        sum_kernel,
        out_shape=struct((tokens, width)),
        in_specs=[VMEM],
        out_specs=VMEM,
        compiler_params=pltpu.CompilerParams(vmem_limit_bytes=6 << 20),
    )(summed)
    return gate_new, up_new, down_new, mixed.T


def solution(mesh):
    placed = (P("fs", "tp"), P("fs"), P("fs", "tp"), P("fs", "tp"), P("fs", "tp"))
    return jax.shard_map(
        on_device,
        mesh=mesh,
        in_specs=placed,
        out_specs=(P("tp", None), P("tp", None), P("tp", None), P("tp", "fs")),
        check_vma=False,
    )
```

```python
import jax
import jax.numpy as jnp
from jax import lax
from jax.experimental import pallas as pl
from jax.experimental.pallas import tpu as pltpu
from jax.sharding import PartitionSpec as P


SIDE = 8
SCALE = 2.0**18
VMEM = pl.BlockSpec(memory_space=pltpu.VMEM)
SMEM = pl.BlockSpec(memory_space=pltpu.SMEM)


def struct(shape, dtype=jnp.bfloat16):
    return jax.ShapeDtypeStruct(shape, dtype)


def strides(core):
    return jnp.where(core == 0, 1, SIDE), jnp.where(core == 0, SIDE, 1)


def lift_kernel(prompt_ref, out_ref):
    out_ref[...] = prompt_ref[...]


def stack_kernel(first_ref, second_ref, out_ref):
    out_ref[0] = first_ref[...]
    out_ref[1] = second_ref[...]


def hidden_kernel(me, *refs):
    pairs, (near_ref, other_ref, mine_ref) = refs[: len(refs) - 3], refs[len(refs) - 3 :]
    chips = len(pairs)
    _, tokens, width = pairs[0].shape
    cols = near_ref.shape[-1] // 3
    core = lax.rem(me[0], 2)
    along_z, along_y = strides(core)

    def weights(slab, columns):
        at = [slab * along_z + y * along_y for y in range(SIDE)]
        return jnp.concatenate([near_ref[row, :, columns] for row in at], axis=0)

    squares = jnp.zeros((tokens, width), jnp.float32)
    for pair in pairs:
        for k in range(2):
            x = pair[k].astype(jnp.float32)
            squares += x * x
    inverse = lax.rsqrt(jnp.sum(squares, axis=1, keepdims=True) / (2 * chips * width) + 1e-06)
    both = 0.0
    for step, pair in enumerate(pairs):
        chip = lax.rem(me[0] // 2 + chips - step, chips)
        for k in range(2):
            normed = (pair[k].astype(jnp.float32) * inverse).astype(jnp.bfloat16)
            slab = 2 * chip + (core if k == 0 else 1 - core)
            both += jnp.dot(normed, weights(slab, slice(0, 2 * cols)), preferred_element_type=jnp.float32)
    gate, up = both[:, :cols], both[:, cols:]
    hidden = (gate / (1 + jnp.exp(-gate)) * up).astype(jnp.bfloat16)

    def share(slab):
        down = weights(slab, slice(2 * cols, 3 * cols))
        return lax.dot_general(hidden, down, (((1,), (1,)), ((), ())), preferred_element_type=jnp.float32)

    for k in range(chips):
        other_ref[k] = share(2 * k + 1 - core).astype(jnp.bfloat16)
        mine_ref[k] = share(2 * k + core)


def pair_kernel(mine_ref, got_ref, out_ref):
    out_ref[...] = (mine_ref[...] + got_ref[...].astype(jnp.float32)).astype(jnp.bfloat16)


def turn_kernel(me, near_ref, *outs):
    cols = outs[0].shape[0]
    along_z, along_y = strides(lax.rem(me[0], 2))
    at = [pl.program_id(0) * along_z + y * along_y for y in range(SIDE)]
    for k, out in enumerate(outs):
        slab = jnp.concatenate([near_ref[row, :, k * cols : (k + 1) * cols] for row in at], axis=0)
        out[...] = slab.T


def sum_kernel(parts_ref, out_ref):
    total = parts_ref[0].astype(jnp.float32)
    for k in range(1, parts_ref.shape[0]):
        total += parts_ref[k].astype(jnp.float32)
    out_ref[...] = total.astype(jnp.bfloat16)


def device(z, y, t, tp):
    return (z * SIDE + y) * tp + t


def lines(tp, even, odd):
    groups = []
    for t in range(tp):
        for o in range(SIDE):
            along = (odd if t % 2 else even) == "y"
            groups.append([device(o, i, t, tp) if along else device(i, o, t, tp) for i in range(SIDE)])
    return groups


def on_device(prompt, norm_gain, gate_master, up_master, down_master):
    tp, fs = lax.axis_size("tp"), lax.axis_size("fs")
    tokens, width = prompt.shape
    rows, cols = gate_master.shape
    every = ("fs", "tp")
    gain_col = norm_gain[:, None]
    parts = [gate_master * gain_col, up_master * gain_col, down_master]
    sent = jnp.concatenate([(lax.reduce_precision(p, 8, 7) * SCALE).astype(jnp.float16) for p in parts], axis=1)
    copies = jnp.broadcast_to(sent, (SIDE, *sent.shape))
    own = lax.all_to_all(copies, every, 0, 0, tiled=True, axis_index_groups=lines(tp, "z", "y"))
    partner = lax.ppermute(prompt, "tp", [(t, t ^ 1) for t in range(tp)])
    own_prompt = pl.pallas_call(
        lift_kernel,
        out_shape=struct((tokens, width)),
        in_specs=[VMEM],
        out_specs=VMEM,
        compiler_params=pltpu.CompilerParams(vmem_limit_bytes=4 << 20),
    )(prompt)
    pairs = [
        pl.pallas_call(
            stack_kernel,
            out_shape=struct((2, tokens, width)),
            in_specs=[VMEM, VMEM],
            out_specs=VMEM,
            compiler_params=pltpu.CompilerParams(vmem_limit_bytes=4 << 20),
        )(own_prompt, partner)
    ]
    for step in range(1, tp // 2):
        pairs.append(lax.ppermute(pairs[0], "tp", [(t, (t + 2 * step) % tp) for t in range(tp)]))
    filled = lax.all_gather(own.reshape(SIDE * rows, 3 * cols), every, axis=0, tiled=True, axis_index_groups=lines(tp, "y", "z"))
    near = (filled.astype(jnp.float32) * (1 / SCALE)).astype(jnp.bfloat16)
    me = lax.axis_index("tp").astype(jnp.int32)[None]
    block = (tp // 2, tokens, width)
    other, mine = pl.pallas_call(
        hidden_kernel,
        out_shape=(struct(block), struct(block, jnp.float32)),
        in_specs=[SMEM] + [VMEM] * (tp // 2 + 1),
        out_specs=(VMEM, VMEM),
        compiler_params=pltpu.CompilerParams(vmem_limit_bytes=16 << 20),
    )(me, *pairs, near.reshape(SIDE * SIDE, rows, 3 * cols))
    got = lax.ppermute(other, "tp", [(t, t ^ 1) for t in range(tp)])
    paired = pl.pallas_call(
        pair_kernel,
        out_shape=struct(block),
        in_specs=[VMEM, VMEM],
        out_specs=VMEM,
        compiler_params=pltpu.CompilerParams(vmem_limit_bytes=8 << 20),
    )(mine, got)
    chips = [[t for t in range(c, tp, 2)] for c in range(2)]
    summed = lax.all_to_all(paired, "tp", 0, 0, tiled=True, axis_index_groups=chips)
    turned = struct((cols, rows * fs))

    gate_new, up_new, down_new = pl.pallas_call(
        turn_kernel,
        out_shape=(turned, turned, turned),
        grid_spec=pltpu.PrefetchScalarGridSpec(
            num_scalar_prefetch=1,
            grid=(SIDE,),
            in_specs=[VMEM],
            out_specs=[pl.BlockSpec((cols, SIDE * rows), lambda z, me: (0, z))] * 3,
        ),
        compiler_params=pltpu.CompilerParams(vmem_limit_bytes=16 << 20),
        cost_estimate=pl.CostEstimate(flops=2 * 10**9, bytes_accessed=12 * rows * fs * cols, transcendentals=0),
    )(me, near.reshape(SIDE * SIDE, rows, 3 * cols))
    mixed = pl.pallas_call(
        sum_kernel,
        out_shape=struct((tokens, width)),
        in_specs=[VMEM],
        out_specs=VMEM,
        compiler_params=pltpu.CompilerParams(vmem_limit_bytes=6 << 20),
    )(summed)
    return gate_new, up_new, down_new, mixed.T


def solution(mesh):
    placed = (P("fs", "tp"), P("fs"), P("fs", "tp"), P("fs", "tp"), P("fs", "tp"))
    return jax.shard_map(
        on_device,
        mesh=mesh,
        in_specs=placed,
        out_specs=(P("tp", None), P("tp", None), P("tp", None), P("tp", "fs")),
        check_vma=False,
    )
```

```python
import jax
import jax.numpy as jnp
from jax import lax
from jax.experimental import pallas as pl
from jax.experimental.pallas import tpu as pltpu
from jax.sharding import PartitionSpec as P


SIDE = 8
SLABS = 4
SCALE = 2.0**18
VMEM = pl.BlockSpec(memory_space=pltpu.VMEM)
SMEM = pl.BlockSpec(memory_space=pltpu.SMEM)


def struct(shape, dtype=jnp.bfloat16):
    return jax.ShapeDtypeStruct(shape, dtype)


def strides(core):
    return jnp.where(core == 0, 1, SIDE), jnp.where(core == 0, SIDE, 1)


def lift_kernel(prompt_ref, out_ref):
    out_ref[...] = prompt_ref[...]


def stack_kernel(first_ref, second_ref, out_ref):
    out_ref[0] = first_ref[...]
    out_ref[1] = second_ref[...]


def hidden_kernel(me, *refs):
    pairs, (near_ref, other_ref, mine_ref) = refs[: len(refs) - 3], refs[len(refs) - 3 :]
    chips = len(pairs)
    _, tokens, width = pairs[0].shape
    cols = near_ref.shape[-1] // 3
    core = lax.rem(me[0], 2)
    along_z, along_y = strides(core)

    def weights(slab, columns):
        at = [slab * along_z + y * along_y for y in range(SIDE)]
        return jnp.concatenate([near_ref[row, :, columns] for row in at], axis=0)

    squares = jnp.zeros((tokens, width), jnp.float32)
    for pair in pairs:
        for k in range(2):
            x = pair[k].astype(jnp.float32)
            squares += x * x
    inverse = lax.rsqrt(jnp.sum(squares, axis=1, keepdims=True) / (2 * chips * width) + 1e-06)
    both = 0.0
    for step, pair in enumerate(pairs):
        chip = lax.rem(me[0] // 2 + chips - step, chips)
        for k in range(2):
            normed = (pair[k].astype(jnp.float32) * inverse).astype(jnp.bfloat16)
            slab = 2 * chip + (core if k == 0 else 1 - core)
            both += jnp.dot(normed, weights(slab, slice(0, 2 * cols)), preferred_element_type=jnp.float32)
    gate, up = both[:, :cols], both[:, cols:]
    hidden = (gate / (1 + jnp.exp(-gate)) * up).astype(jnp.bfloat16)

    def share(slab):
        down = weights(slab, slice(2 * cols, 3 * cols))
        return lax.dot_general(hidden, down, (((1,), (1,)), ((), ())), preferred_element_type=jnp.float32)

    for k in range(chips):
        other_ref[k] = share(2 * k + 1 - core).astype(jnp.bfloat16)
        mine_ref[k] = share(2 * k + core)


def pair_kernel(mine_ref, got_ref, out_ref):
    out_ref[...] = (mine_ref[...] + got_ref[...].astype(jnp.float32)).astype(jnp.bfloat16)


def turn_kernel(me, near_ref, *outs):
    cols = outs[0].shape[0]
    along_z, along_y = strides(lax.rem(me[0], 2))
    zs = [pl.program_id(0) * SLABS + k for k in range(SLABS)]
    at = [z * along_z + y * along_y for z in zs for y in range(SIDE)]
    for k, out in enumerate(outs):
        slab = jnp.concatenate([near_ref[row, :, k * cols : (k + 1) * cols] for row in at], axis=0)
        out[...] = slab.T


def sum_kernel(parts_ref, out_ref):
    total = parts_ref[0].astype(jnp.float32)
    for k in range(1, parts_ref.shape[0]):
        total += parts_ref[k].astype(jnp.float32)
    out_ref[...] = total.astype(jnp.bfloat16)


def device(z, y, t, tp):
    return (z * SIDE + y) * tp + t


def lines(tp, even, odd):
    groups = []
    for t in range(tp):
        for o in range(SIDE):
            along = (odd if t % 2 else even) == "y"
            groups.append([device(o, i, t, tp) if along else device(i, o, t, tp) for i in range(SIDE)])
    return groups


def on_device(prompt, norm_gain, gate_master, up_master, down_master):
    tp, fs = lax.axis_size("tp"), lax.axis_size("fs")
    tokens, width = prompt.shape
    rows, cols = gate_master.shape
    every = ("fs", "tp")
    gain_col = norm_gain[:, None]
    parts = [gate_master * gain_col, up_master * gain_col, down_master]
    sent = jnp.concatenate([(lax.reduce_precision(p, 8, 7) * SCALE).astype(jnp.float16) for p in parts], axis=1)
    copies = jnp.broadcast_to(sent, (SIDE, *sent.shape))
    own = lax.all_to_all(copies, every, 0, 0, tiled=True, axis_index_groups=lines(tp, "z", "y"))
    partner = lax.ppermute(prompt, "tp", [(t, t ^ 1) for t in range(tp)])
    own_prompt = pl.pallas_call(
        lift_kernel,
        out_shape=struct((tokens, width)),
        in_specs=[VMEM],
        out_specs=VMEM,
        compiler_params=pltpu.CompilerParams(vmem_limit_bytes=4 << 20),
    )(prompt)
    pairs = [
        pl.pallas_call(
            stack_kernel,
            out_shape=struct((2, tokens, width)),
            in_specs=[VMEM, VMEM],
            out_specs=VMEM,
            compiler_params=pltpu.CompilerParams(vmem_limit_bytes=4 << 20),
        )(own_prompt, partner)
    ]
    for step in range(1, tp // 2):
        pairs.append(lax.ppermute(pairs[0], "tp", [(t, (t + 2 * step) % tp) for t in range(tp)]))
    filled = lax.all_gather(own.reshape(SIDE * rows, 3 * cols), every, axis=0, tiled=True, axis_index_groups=lines(tp, "y", "z"))
    near = (filled.astype(jnp.float32) * (1 / SCALE)).astype(jnp.bfloat16)
    me = lax.axis_index("tp").astype(jnp.int32)[None]
    block = (tp // 2, tokens, width)
    other, mine = pl.pallas_call(
        hidden_kernel,
        out_shape=(struct(block), struct(block, jnp.float32)),
        in_specs=[SMEM] + [VMEM] * (tp // 2 + 1),
        out_specs=(VMEM, VMEM),
        compiler_params=pltpu.CompilerParams(vmem_limit_bytes=16 << 20),
    )(me, *pairs, near.reshape(SIDE * SIDE, rows, 3 * cols))
    got = lax.ppermute(other, "tp", [(t, t ^ 1) for t in range(tp)])
    paired = pl.pallas_call(
        pair_kernel,
        out_shape=struct(block),
        in_specs=[VMEM, VMEM],
        out_specs=VMEM,
        compiler_params=pltpu.CompilerParams(vmem_limit_bytes=8 << 20),
    )(mine, got)
    chips = [[t for t in range(c, tp, 2)] for c in range(2)]
    summed = lax.all_to_all(paired, "tp", 0, 0, tiled=True, axis_index_groups=chips)
    turned = struct((cols, rows * fs))

    gate_new, up_new, down_new = pl.pallas_call(
        turn_kernel,
        out_shape=(turned, turned, turned),
        grid_spec=pltpu.PrefetchScalarGridSpec(
            num_scalar_prefetch=1,
            grid=(SIDE // SLABS,),
            in_specs=[VMEM],
            out_specs=[pl.BlockSpec((cols, SLABS * SIDE * rows), lambda z, me: (0, z))] * 3,
        ),
        compiler_params=pltpu.CompilerParams(vmem_limit_bytes=16 << 20),
        cost_estimate=pl.CostEstimate(flops=2 * 10**9, bytes_accessed=12 * rows * fs * cols, transcendentals=0),
    )(me, near.reshape(SIDE * SIDE, rows, 3 * cols))
    mixed = pl.pallas_call(
        sum_kernel,
        out_shape=struct((tokens, width)),
        in_specs=[VMEM],
        out_specs=VMEM,
        compiler_params=pltpu.CompilerParams(vmem_limit_bytes=6 << 20),
    )(summed)
    return gate_new, up_new, down_new, mixed.T


def solution(mesh):
    placed = (P("fs", "tp"), P("fs"), P("fs", "tp"), P("fs", "tp"), P("fs", "tp"))
    return jax.shard_map(
        on_device,
        mesh=mesh,
        in_specs=placed,
        out_specs=(P("tp", None), P("tp", None), P("tp", None), P("tp", "fs")),
        check_vma=False,
    )
```
